32 devices in a mesh: sp: 8 (over z, core), tp: 4 (over y, x).
Axes of the slice: x: 2, y: 2, z: 4, core: 2. Of those that a mesh axis runs over, the one named last changes fastest.
Arguments:
- query_a: bfloat16 [1536, 2048], P('sp', 'tp'), may hold values from -6 to 6
- key_a: bfloat16 [1536, 2048], P('sp', 'tp'), may hold values from -6 to 6
- value_a: bfloat16 [1536, 2048], P('sp', 'tp'), may hold values from -6 to 6
- query_b: bfloat16 [1536, 2048], P('sp', 'tp'), may hold values from -6 to 6
- key_b: bfloat16 [1536, 2048], P('sp', 'tp'), may hold values from -6 to 6
- value_b: bfloat16 [1536, 2048], P('sp', 'tp'), may hold values from -6 to 6
- stop_a: float32 [1536, 32], P('sp', 'tp'), may hold values from -14 to -1
- stop_b: float32 [1536, 16], P('sp', 'tp'), may hold values from -14 to -1
- out_a: bfloat16 [2048, 2048], P('tp'), may hold values from -4 to 4
- out_b: bfloat16 [2048, 2048], P('tp'), may hold values from -4 to 4
- resid: bfloat16 [1536, 2048], P('sp', 'tp'), may hold values from -20 to 20
- mix_gain: float32 [2048], P('tp'), may hold values from 0.1 to 1.9
- ffn_gain: float32 [2048], P('tp'), may hold values from 0.1 to 1.9
- routes: int32 [1536, 2], P('sp'), may hold values from 0 to 31, all different within a row; in each aligned block of 192 rows (0 to 191, 192 to 383, ...) at most 18 rows name the same one
- gates: float32 [1536, 2], P('sp'), may hold values from 0.25 to 1.5
- exp_gate: bfloat16 [32, 2048, 512], P('sp', 'tp'), may hold values from -0.125 to 0.125
- exp_up: bfloat16 [32, 2048, 512], P('sp', 'tp'), may hold values from -0.125 to 0.125
- exp_down: bfloat16 [32, 512, 2048], P('sp', None, 'tp'), may hold values from -0.25 to 0.25
- sh_gate: bfloat16 [2048, 512], P('tp'), may hold values from -0.125 to 0.125
- sh_up: bfloat16 [2048, 512], P('tp'), may hold values from -0.125 to 0.125
- sh_down: bfloat16 [512, 2048], P(None, 'tp'), may hold values from -4 to 4
Outputs:
- result: bfloat16 [1536, 2048], P('sp', 'tp')
The draws below stay inside these ranges and needn't reach their ends.
Inputs may be any that keep to these rules, and one draw needn't show every extreme that they name: `routes`: each row names 2 different experts. Within the rows of one index of sp (aligned blocks of 192 rows) no expert is named by more than 18 rows, a bound that some block reaches.
All inputs are finite; a program needn't handle non-finite values.
Results may differ from the reference program's by a relative error of at most 0.02.
Values may be sent and summed in bfloat16 or wider, within the bound.
No kernel may reach another device: no remote copies, remote signals or barrier semaphores. Data moves between devices by JAX's collectives and lax.ppermute only.
A program may use at most 64 MiB of HBM per device.

```python
import math
import jax
import jax.numpy as jnp
import numpy as np
from jax import lax

D = 2048
HA = 32
HEAD_A = 64
HB = 16
HEAD_B = 128
F = 512
FS = 512
TOP_K = 2
TOK = 192
TOKENS = 1536
EXPERTS = 32
CAP = 18
N_SP = 8
N_TP = 4


def column_scales(key, columns):
    width = max(1, columns // 32)
    count = (columns + width - 1) // width
    levels = jnp.exp(jax.random.uniform(key, (count,), jnp.float32, math.log(0.33), math.log(3.0)))
    return levels[jnp.arange(columns) // width]


def scaled_normal(key, rows, columns, spread, scale_key):
    values = jnp.clip(jax.random.normal(key, (rows, columns), jnp.float32), -5.0, 5.0) * spread
    return values * column_scales(scale_key, columns)[None, :]


def stop_offsets(key, heads):
    parts = jax.random.split(key, 5)
    chance = jax.random.uniform(parts[0], (heads,), jnp.float32)
    slow = chance < 0.5
    base = jnp.where(slow, -math.log(TOKENS) - 0.5, -4.0)
    base = base + jax.random.uniform(parts[1], (heads,), jnp.float32, -0.5, 0.5)
    phase = jax.random.uniform(parts[2], (heads,), jnp.float32, 0.0, 2.0 * math.pi)
    position = jnp.arange(TOKENS, dtype=jnp.float32) / TOKENS
    trend = 0.8 * jnp.sin(6.0 * math.pi * position[:, None] + phase[None, :])
    count = (TOKENS + 7) // 8
    jitter = jax.random.uniform(parts[3], (count, heads), jnp.float32, -0.8, 0.8)[jnp.arange(TOKENS) // 8]
    rough = jax.random.uniform(parts[4], (TOKENS, heads), jnp.float32, -0.3, 0.3)
    return base[None, :] + trend + jitter + rough


def draw_stop_a(key, part):
    return stop_offsets(jax.random.fold_in(key, 21), HA)


def draw_stop_b(key, part):
    return stop_offsets(jax.random.fold_in(key, 22), HB)


def draw_out_a(key, part):
    spread = (HA * HEAD_A + HB * HEAD_B) ** (-0.5)
    values = scaled_normal(jax.random.fold_in(key, 31), HA * HEAD_A, D, spread, jax.random.fold_in(key, 7))
    return values.astype(jnp.bfloat16)


def draw_out_b(key, part):
    spread = (HA * HEAD_A + HB * HEAD_B) ** (-0.5)
    values = scaled_normal(jax.random.fold_in(key, 32), HB * HEAD_B, D, spread, jax.random.fold_in(key, 7))
    return values.astype(jnp.bfloat16)


def draw_resid(key, part):
    values = scaled_normal(jax.random.fold_in(key, 41), TOKENS, D, 1.0, jax.random.fold_in(key, 5))
    return values.astype(jnp.bfloat16)


def draw_sh_down(key, part):
    values = scaled_normal(jax.random.fold_in(key, 51), FS, D, FS ** (-0.5), jax.random.fold_in(key, 9))
    return values.astype(jnp.bfloat16)


def block_scale(stream_key, shape, cuts, least, top_value):
    def one(dim, blocks):
        heights = jax.random.uniform(jax.random.fold_in(jax.random.fold_in(stream_key, 6), dim), (blocks,), jnp.float32, least / len(cuts), top_value / len(cuts))
        return jnp.repeat(jnp.exp(heights), shape[dim] // blocks).reshape((-1,) + (1,) * (len(shape) - dim - 1))

    factor_of = one(*cuts[0])
    for cut in cuts[1:]:
        factor_of = factor_of * one(*cut)
    return factor_of


def deal_out(rng, own, number, rows, number_of, top, reach, skew):
    order = jax.random.permutation(rng, number_of)
    packed, ordinary = load_shares(number_of, rows * top, reach, skew, True), load_shares(number_of, rows * top, reach, skew, False)
    places = jnp.arange(number_of)

    def named(tallies, turn):
        used = int((tallies > 0).sum())
        fixed = max(1, used // 4)
        moved = fixed + (places - fixed + turn * (used - fixed)) % max(1, number_of - fixed)
        return jnp.zeros((number_of,), jnp.int32).at[order[jnp.where(places < fixed, places, moved)]].set(jnp.asarray(tallies, jnp.int32))

    tallies = jnp.where(number % 4 == 0, named(packed, number // 4), named(ordinary, number - number // 4 - 1))
    mixed = jax.random.permutation(jax.random.fold_in(own, 3), number_of)
    source_of, sink = mixed[0:number_of // 2 * 2:2], mixed[1:number_of // 2 * 2:2]
    slack = jnp.minimum(tallies[source_of] - 1, reach - tallies[sink]) // 2
    slack = jnp.where((source_of == order[0]) | (sink == order[0]) | (tallies[sink] == 0), 0, jnp.maximum(slack, 0))
    moved = jax.random.randint(jax.random.fold_in(own, 4), (number_of // 2,), 0, 1 << 20) % (slack + 1)
    tallies = tallies.at[source_of].add(-moved).at[sink].add(moved)
    labels = jnp.searchsorted(jnp.cumsum(tallies), jnp.arange(rows * top), side="right").astype(jnp.int32)
    grid = labels.reshape(top, rows).T
    grid = grid[jax.random.permutation(jax.random.fold_in(own, 1), rows)]
    turn = jax.random.randint(jax.random.fold_in(own, 2), (rows, 1), 0, top)
    return jnp.take_along_axis(grid, (jnp.arange(top)[None, :] + turn) % top, axis=1)


def load_shares(number_of, total, reach, slope, full):
    weights = [(1 << 20) // math.isqrt(standing ** slope) + 1 for standing in range(1, number_of + 1)]
    largest = reach if full else min(reach, max(-(-total // number_of), total * weights[0] // sum(weights)))
    least = 1 if total - largest >= number_of - 1 else 0
    given, surplus = [largest] + [least] * (number_of - 1), total - largest - least * (number_of - 1)
    while surplus > 0:
        movable = [i for i in range(1, number_of) if given[i] < largest] or [i for i in range(1, number_of) if given[i] < reach]
        pool, budget = sum([weights[i] for i in movable]), surplus
        for i in movable:
            more = min(reach - given[i], max(1, budget * weights[i] // pool), surplus)
            given[i] = given[i] + more
            surplus = surplus - more
    return np.array(given)


def scatter_about(stream_key, extent, deviation, most, cuts=(), kind=jnp.bfloat16):
    array = deviation * jax.random.normal(stream_key, extent, jnp.float32)
    if cuts:
        array = array * block_scale(stream_key, extent, cuts, -0.22, 0.18)
    return jnp.clip(array, -most, most).astype(kind)


def setup_inputs(seed: int = 0) -> dict:
    seeds = jax.random.split(jax.random.key(seed), 22)
    query_a = scatter_about(seeds[0], (TOKENS, HA * HEAD_A), 1.0, 6.0, ((0, 8), (1, 4)))
    key_a = scatter_about(seeds[1], (TOKENS, HA * HEAD_A), 1.0, 6.0, ((0, 8), (1, 4)))
    value_a = scatter_about(seeds[2], (TOKENS, HA * HEAD_A), 1.0, 6.0, ((0, 8), (1, 4)))
    query_b = scatter_about(seeds[3], (TOKENS, HB * HEAD_B), 1.0, 6.0, ((0, 8), (1, 4)))
    key_b = scatter_about(seeds[4], (TOKENS, HB * HEAD_B), 1.0, 6.0, ((0, 8), (1, 4)))
    value_b = scatter_about(seeds[5], (TOKENS, HB * HEAD_B), 1.0, 6.0, ((0, 8), (1, 4)))
    stop_a = draw_stop_a(jax.random.fold_in(seeds[21], 71), 0)
    stop_b = draw_stop_b(jax.random.fold_in(seeds[21], 71), 0)
    out_a = draw_out_a(jax.random.fold_in(seeds[21], 71), 0)
    out_b = draw_out_b(jax.random.fold_in(seeds[21], 71), 0)
    resid = draw_resid(jax.random.fold_in(seeds[21], 71), 0)
    mix_gain = jnp.clip(1.0 + 0.18 * jax.random.normal(seeds[11], (D,), jnp.float32), 0.1, 1.9)
    ffn_gain = jnp.clip(1.0 + 0.18 * jax.random.normal(seeds[12], (D,), jnp.float32), 0.1, 1.9)
    routes_keys = jax.random.split(jax.random.fold_in(seeds[13], 1), TOKENS // TOK)
    routes_turns = jax.random.permutation(jax.random.fold_in(seeds[13], 3), TOKENS // TOK)
    routes = jax.vmap(lambda own, number: deal_out(jax.random.fold_in(seeds[13], 2), own, number, TOK, EXPERTS, TOP_K, CAP, 1))(routes_keys, routes_turns).reshape((TOKENS, TOP_K))
    gates = jnp.clip(0.25 + 1.25 * jax.random.uniform(seeds[14], (TOKENS, TOP_K), jnp.float32) ** block_scale(seeds[14], (TOKENS, TOP_K), ((0, 8),), -0.2, 0.2), 0.25, 1.5)
    exp_gate = scatter_about(seeds[15], (EXPERTS, D, F), D ** -0.5, 0.125, ((0, 8), (1, 4)))
    exp_up = scatter_about(seeds[16], (EXPERTS, D, F), D ** -0.5, 0.125, ((0, 8), (1, 4)))
    exp_down = scatter_about(seeds[17], (EXPERTS, F, D), F ** -0.5, 0.25, ((0, 8), (2, 4)))
    sh_gate = scatter_about(seeds[18], (D, FS), D ** -0.5, 0.125, ((0, 4),))
    sh_up = scatter_about(seeds[19], (D, FS), D ** -0.5, 0.125, ((0, 4),))
    sh_down = draw_sh_down(jax.random.fold_in(seeds[21], 71), 0)
    return {"query_a": query_a, "key_a": key_a, "value_a": value_a, "query_b": query_b, "key_b": key_b, "value_b": value_b, "stop_a": stop_a, "stop_b": stop_b, "out_a": out_a, "out_b": out_b, "resid": resid, "mix_gain": mix_gain, "ffn_gain": ffn_gain, "routes": routes, "gates": gates, "exp_gate": exp_gate, "exp_up": exp_up, "exp_down": exp_down, "sh_gate": sh_gate, "sh_up": sh_up, "sh_down": sh_down}


epsilon = 1e-06

def stick_group(query, keys, values, stop, heads):
    size = query.shape[1] // heads
    scale = size ** (-0.5)
    blocks = TOKENS // TOK
    query_blocks = query.reshape(blocks, TOK, heads, size).astype(jnp.float32)
    key_blocks = keys.reshape(blocks, TOK, heads, size).astype(jnp.float32)
    value_blocks = values.reshape(blocks, TOK, heads, size).astype(jnp.float32)
    stop_blocks = stop.reshape(blocks, TOK, heads).astype(jnp.float32)
    places = jnp.arange(TOK, dtype=jnp.int32)

    def one_query_block(number):
        query_here = query_blocks[number]
        stop_here = jnp.transpose(stop_blocks[number])[:, :, None]

        def visit(offset, state):
            source = number - offset

            def work(inner):
                output, carried = inner
                safe = jnp.maximum(source, 0)
                key_here = key_blocks[safe]
                value_here = value_blocks[safe]
                scores = jnp.einsum('qhd,khd->hqk', query_here, key_here, precision=lax.Precision.HIGHEST) * scale + stop_here
                causal = (source * TOK + places)[None, :] < (number * TOK + places)[:, None]
                failing = jnp.where(causal[None], jax.nn.log_sigmoid(-scores), 0.0)
                after = lax.cumsum(failing, axis=2, reverse=True) - failing + carried[:, :, None]
                weight = jnp.where(causal[None], jnp.exp(jax.nn.log_sigmoid(scores) + after), 0.0)
                weight = lax.optimization_barrier(weight.astype(jnp.bfloat16)).astype(jnp.float32)
                output = output + jnp.einsum('hqk,khe->qhe', weight, value_here, precision=lax.Precision.HIGHEST)
                return (output, carried + lax.optimization_barrier(jnp.sum(failing, axis=2)))
            return lax.cond(source >= 0, work, lambda inner: inner, state)
        start = (jnp.zeros((TOK, heads, size), jnp.float32), jnp.zeros((heads, TOK), jnp.float32))
        output, _ = lax.fori_loop(0, blocks, visit, start)
        return output
    gathered = lax.map(one_query_block, jnp.arange(blocks, dtype=jnp.int32))
    return gathered.reshape(TOKENS, heads * size).astype(jnp.bfloat16)

def grouped_product(rows, weight):
    count = rows.shape[0]
    width = weight.shape[1]
    part_rows = rows.reshape(count, N_TP, D // N_TP).astype(jnp.float32)
    part_weight = weight.reshape(N_TP, D // N_TP, width).astype(jnp.float32)
    partial_value = jnp.einsum('rgd,gdf->grf', part_rows, part_weight, precision=lax.Precision.HIGHEST)
    rounded = lax.optimization_barrier(partial_value.astype(jnp.bfloat16))
    return lax.optimization_barrier(jnp.sum(rounded.astype(jnp.float32), axis=0))

def row_scale(values):
    return lax.rsqrt(lax.optimization_barrier(jnp.mean(values * values, axis=1, keepdims=True)) + epsilon)

def reference(query_a, key_a, value_a, query_b, key_b, value_b, stop_a, stop_b, out_a, out_b, resid, mix_gain, ffn_gain, routes, gates, exp_gate, exp_up, exp_down, sh_gate, sh_up, sh_down):
    attended_a = stick_group(query_a, key_a, value_a, stop_a, HA)
    attended_b = stick_group(query_b, key_b, value_b, stop_b, HB)
    rows_a = HA * HEAD_A // N_TP
    rows_b = HB * HEAD_B // N_TP
    sets_a = jnp.transpose(attended_a.reshape(TOKENS, N_TP, rows_a), (1, 0, 2))
    sets_b = jnp.transpose(attended_b.reshape(TOKENS, N_TP, rows_b), (1, 0, 2))
    weights_a = out_a.reshape(N_TP, rows_a, D)
    weights_b = out_b.reshape(N_TP, rows_b, D)

    def add_set(total, pieces):
        left_a, right_a, left_b, right_b = pieces
        partial_value = jnp.dot(left_a, right_a, preferred_element_type=jnp.float32)
        partial_value = partial_value + jnp.dot(left_b, right_b, preferred_element_type=jnp.float32)
        return (total + lax.optimization_barrier(partial_value.astype(jnp.bfloat16)).astype(jnp.float32), None)
    mixed, _ = lax.scan(add_set, jnp.zeros((TOKENS, D), jnp.float32), (sets_a, weights_a, sets_b, weights_b))
    branch = mixed * row_scale(mixed) * mix_gain.astype(jnp.float32)[None, :]
    stream = lax.optimization_barrier((resid.astype(jnp.float32) + branch).astype(jnp.bfloat16))
    stream_f = stream.astype(jnp.float32)
    normed = (stream_f * row_scale(stream_f) * ffn_gain.astype(jnp.float32)[None, :]).astype(jnp.bfloat16)
    pairs = routes.reshape(N_SP, TOK * TOP_K).astype(jnp.int32)
    onehot = (pairs[:, :, None] == jnp.arange(EXPERTS, dtype=jnp.int32)[None, None, :]).astype(jnp.int32)
    earlier = jnp.cumsum(onehot, axis=1) - onehot
    ranks = lax.optimization_barrier(jnp.sum(earlier * onehot, axis=2))
    group = jnp.arange(N_SP, dtype=jnp.int32)[:, None]
    index = ((pairs * N_SP + group) * CAP + ranks).reshape(-1).astype(jnp.int32)
    source_rows = jnp.repeat(jnp.arange(TOKENS, dtype=jnp.int32), TOP_K)
    buffer = jnp.zeros((EXPERTS * N_SP * CAP, D), jnp.bfloat16).at[index].set(normed[source_rows])
    buffer = buffer.reshape(EXPERTS, N_SP * CAP, D)

    def one_expert(pieces):
        rows_here, gate_here, up_here, down_here = pieces
        gate_pre = grouped_product(rows_here, gate_here)
        up_pre = grouped_product(rows_here, up_here)
        hidden = (jax.nn.silu(gate_pre) * up_pre).astype(jnp.bfloat16)
        return jnp.dot(hidden, down_here, preferred_element_type=jnp.float32).astype(jnp.bfloat16)
    produced = lax.map(one_expert, (buffer, exp_gate, exp_up, exp_down)).reshape(EXPERTS * N_SP * CAP, D)
    picked = produced[index].reshape(TOKENS, TOP_K, D).astype(jnp.float32)
    routed = lax.optimization_barrier(jnp.sum(gates.astype(jnp.float32)[:, :, None] * picked, axis=1))
    shared_gate = grouped_product(normed, sh_gate)
    shared_up = grouped_product(normed, sh_up)
    shared_hidden = (jax.nn.silu(shared_gate) * shared_up).astype(jnp.bfloat16)
    shared_out = jnp.dot(shared_hidden, sh_down, preferred_element_type=jnp.float32)
    moe = routed + shared_out
    result = stream_f + moe
    return result.astype(jnp.bfloat16)
```

```python
import math

import jax
import jax.numpy as jnp
from jax import lax
from jax.experimental import pallas as pl
from jax.experimental.pallas import tpu as pltpu
from jax.sharding import PartitionSpec as P

epsilon = 1e-06
LOG2E = math.log2(math.e)


class Group:
    def __init__(self, rows, width, heads):
        self.rows = rows
        self.width = width
        self.heads = heads
        self.size = width // heads
        self.pack = 2 if heads % 2 == 0 else 1
        self.sets = heads // self.pack
        self.lanes = self.pack * rows
        self.columns = self.pack * self.size
        self.joint = self.pack == 1 or self.columns <= 128
        if self.joint:
            self.windows = ((0, 0, self.lanes),)
            self.out_rows = self.columns
        else:
            self.windows = tuple(
                (i, (i * rows) // 128 * 128, min(self.lanes, -(-((i + 1) * rows) // 128) * 128))
                for i in range(self.pack)
            )
            self.out_rows = self.size
        self.out_lanes = max(high - low for _, low, high in self.windows)
        self.state_shape = (self.sets * len(self.windows), self.out_rows, self.out_lanes)
        self.carry_shape = (self.sets, 8, self.lanes)


def attention_call(group, flags, query, stop, near, far, state, first, last):
    rows, size, columns, lanes = group.rows, group.size, group.columns, group.lanes
    width = group.width
    steps = rows // 8
    scale = size**-0.5 * LOG2E

    def kernel(*refs):
        refs = list(refs)
        flag_ref, q_ref, stop_ref, x_ref, y_ref = refs[:5]
        del refs[:5]
        if not first:
            acc_in, carry_in = refs[:2]
            del refs[:2]
        if last:
            att_ref = refs.pop(0)
        else:
            acc_out, carry_out = refs[:2]
            del refs[:2]
        kv, q_block, score, weight = refs[:4]
        del refs[:4]
        if last:
            acc, carry = refs[:2]
            del refs[:2]
        else:
            acc, carry = acc_out, carry_out
        sem = refs[0]
        x_slot = flag_ref[0]
        loads = [
            pltpu.make_async_copy(x_ref, kv.at[x_slot], sem.at[0]),
            pltpu.make_async_copy(y_ref, kv.at[1 - x_slot], sem.at[1]),
        ]
        for load in loads:
            load.start()
        lane_q = lax.broadcasted_iota(jnp.int32, (rows, columns), 1)
        for g in range(group.sets):
            part = q_ref[:, g * columns : (g + 1) * columns]
            for i in range(group.pack):
                own = (lane_q >= i * size) & (lane_q < (i + 1) * size)
                q_block[g, i * rows : (i + 1) * rows, :] = jnp.where(own, part, jnp.zeros_like(part))
        if first:
            acc[...] = jnp.zeros(group.state_shape, jnp.float32)
            carry[...] = jnp.zeros(group.carry_shape, jnp.float32)
        else:
            acc[...] = acc_in[...]
            carry[...] = carry_in[...]
        for load in loads:
            load.wait()
        sub = lax.broadcasted_iota(jnp.int32, (8, lanes), 0)

        def block(slot, g, masked):
            keys = kv[slot, :, g * columns : (g + 1) * columns]
            values = kv[slot, :, width + g * columns : width + (g + 1) * columns]
            score[...] = lax.dot_general(
                keys, q_block[g], (((1,), (1,)), ((), ())), preferred_element_type=jnp.float32
            )
            offset = stop_ref[g]
            running = jnp.zeros((8, lanes), jnp.float32)
            if masked:
                place = lax.broadcasted_iota(jnp.int32, (8, lanes), 1) % rows - sub * steps
            for v in reversed(range(steps)):
                z = score[8 * v : 8 * v + 8, :] * scale + offset
                failing = jnp.maximum(z, 0.0) + jnp.log2(1.0 + jnp.exp2(-jnp.abs(z)))
                chance = z - failing - running
                if masked:
                    causal = place > v
                    failing = jnp.where(causal, failing, 0.0)
                    chance = jnp.where(causal, chance, -1e30)
                score[8 * v : 8 * v + 8, :] = chance
                running = running + failing
            later = running
            for shift in (1, 2, 4):
                later = later + jnp.where(sub < 8 - shift, pltpu.roll(later, 8 - shift, 0), 0.0)
            base = carry[g]
            carry[g] = base + jnp.broadcast_to(later[0:1, :], (8, lanes))
            base = base + later - running
            base = jnp.concatenate([base, base], axis=0)
            for v in range(rows // 16):
                weight[16 * v : 16 * v + 16, :] = jnp.exp2(
                    score[16 * v : 16 * v + 16, :] - base
                ).astype(jnp.bfloat16)
            for n, (i, low, high) in enumerate(group.windows):
                chosen = values if group.joint else values[:, i * size : (i + 1) * size]
                at = g * len(group.windows) + n
                acc[at, :, : high - low] += lax.dot_general(
                    chosen,
                    weight[:, low:high],
                    (((0,), (0,)), ((), ())),
                    preferred_element_type=jnp.float32,
                )

        if first:
            for g in range(group.sets):
                block(0, g, True)

            @pl.when(flag_ref[1] > 0)
            def _():
                for g in range(group.sets):
                    block(1, g, False)
        else:

            @pl.when(flag_ref[1] > 0)
            def _():
                def one(slot, _):
                    for g in range(group.sets):
                        block(slot, g, False)
                    return 0

                lax.fori_loop(0, 2, one, 0)

        if last:
            for g in range(group.sets):
                if group.joint:
                    turned = jnp.transpose(acc[g])
                    if group.pack == 1:
                        piece = turned
                    else:
                        piece = turned[:rows, :]
                        for i in range(1, group.pack):
                            piece = jnp.where(
                                lane_q < i * size, piece, turned[i * rows : (i + 1) * rows, :]
                            )
                    att_ref[:, g * columns : (g + 1) * columns] = piece.astype(jnp.bfloat16)
                else:
                    for n, (i, low, high) in enumerate(group.windows):
                        turned = jnp.transpose(acc[g * len(group.windows) + n])
                        begin = i * rows - low
                        start = g * columns + i * size
                        att_ref[:, start : start + size] = turned[begin : begin + rows, :].astype(
                            jnp.bfloat16
                        )

    vmem = pl.BlockSpec(memory_space=pltpu.VMEM)
    anywhere = pl.BlockSpec(memory_space=pl.ANY)
    state_types = (
        jax.ShapeDtypeStruct(group.state_shape, jnp.float32),
        jax.ShapeDtypeStruct(group.carry_shape, jnp.float32),
    )
    args = [flags, query, stop, near, far]
    specs = [pl.BlockSpec(memory_space=pltpu.SMEM), vmem, vmem, anywhere, anywhere]
    if not first:
        args += list(state)
        specs += [vmem, vmem]
    scratch = [
        pltpu.VMEM((2, rows, 2 * width), jnp.bfloat16),
        pltpu.VMEM((group.sets, lanes, columns), jnp.bfloat16),
        pltpu.VMEM((rows, lanes), jnp.float32),
        pltpu.VMEM((rows, lanes), jnp.bfloat16),
    ]
    if last:
        out_shape = jax.ShapeDtypeStruct((rows, width), jnp.bfloat16)
        out_specs = vmem
        scratch += [
            pltpu.VMEM(group.state_shape, jnp.float32),
            pltpu.VMEM(group.carry_shape, jnp.float32),
        ]
    else:
        out_shape = state_types
        out_specs = (vmem, vmem)
    scratch.append(pltpu.SemaphoreType.DMA((2,)))
    elements = 2 * rows * rows * group.heads
    return pl.pallas_call(
        kernel,
        in_specs=specs,
        out_specs=out_specs,
        out_shape=out_shape,
        scratch_shapes=scratch,
        cost_estimate=pl.CostEstimate(
            flops=4 * elements * size, transcendentals=3 * elements, bytes_accessed=8 * rows * width
        ),
    )(*args)


def exchange(parts, axis, count):
    arrived = [parts[0]]
    for d in range(1, count):
        arrived.append(lax.ppermute(parts[d], axis, [(i, (i + d) % count) for i in range(count)]))
    return arrived


def shards(
    query_a,
    key_a,
    value_a,
    query_b,
    key_b,
    value_b,
    stop_a,
    stop_b,
    out_a,
    out_b,
    resid,
    mix_gain,
    ffn_gain,
    routes,
    gates,
    exp_gate,
    exp_up,
    exp_down,
    sh_gate,
    sh_up,
    sh_down,
):
    f32, bf16 = jnp.float32, jnp.bfloat16
    rows = query_a.shape[0]
    n_sp = lax.axis_size("sp")
    n_tp = lax.axis_size("tp")
    position = lax.axis_index("sp")
    member = lax.axis_index("tp")
    core = position % 2
    chip = position // 2
    chips = n_sp // 2

    at = jnp.arange(rows)
    source = (at % 8) * (rows // 8) + at // 8
    shuffle = (source[:, None] == at[None, :]).astype(bf16)
    partner = [(i, i ^ 1) for i in range(n_sp)]
    attended = []
    streams = []
    for query, key, value, stop in (
        (query_a, key_a, value_a, stop_a),
        (query_b, key_b, value_b, stop_b),
    ):
        group = Group(rows, query.shape[1], stop.shape[1])
        own = jnp.dot(
            shuffle, jnp.concatenate([key, value], axis=1), preferred_element_type=f32
        ).astype(bf16)
        lanes = jnp.transpose(stop * LOG2E).reshape(group.sets, 1, group.lanes)
        lanes = jnp.broadcast_to(lanes, (group.sets, 8, group.lanes))
        streams.append((group, query, lanes, own))
    chains = []
    for group, query, lanes, own in streams:
        near = [own]
        far = [lax.ppermute(own, "sp", partner)]
        for r in range(1, chips):
            hop = [(i, i + 2) for i in range(2 * (r - 1), n_sp - 2)]
            near.append(lax.ppermute(near[-1], "sp", hop))
            far.append(lax.ppermute(near[-1], "sp", partner))
        chains.append((near, far))
    for (group, query, lanes, own), (near, far) in zip(streams, chains):
        state = None
        for r in range(chips):
            first, last = r == 0, r == chips - 1
            if first:
                flags = jnp.stack([jnp.zeros_like(core), core])
            else:
                flags = jnp.stack([1 - core, (chip >= r).astype(jnp.int32)])
            state = attention_call(
                group, flags.astype(jnp.int32), query, lanes, near[r], far[r], state, first, last
            )
        attended.append(state)

    partial = jnp.dot(attended[0], out_a, preferred_element_type=f32)
    partial = (partial + jnp.dot(attended[1], out_b, preferred_element_type=f32)).astype(bf16)

    def spread(array, axis):
        part = array.shape[axis] // n_tp
        return [
            lax.dynamic_slice_in_dim(array, (member + d) % n_tp * part, part, axis)
            for d in range(n_tp)
        ]

    def summed(array, axis):
        total = None
        for piece in exchange(spread(array, axis), "tp", n_tp):
            piece = piece.astype(f32)
            total = piece if total is None else total + piece
        return total

    def joined(array, axis):
        return lax.all_gather(array, "tp", axis=axis, tiled=True)

    mixed = summed(partial, 1)
    resid_f = resid.astype(f32)
    gained = mixed * mix_gain[None, :]
    sums = jnp.stack(
        [
            jnp.sum(mixed * mixed, axis=1),
            jnp.sum(gained * gained, axis=1),
            jnp.sum(gained * resid_f, axis=1),
            jnp.sum(resid_f * resid_f, axis=1),
        ]
    )
    sums = sum(exchange([sums] * n_tp, "tp", n_tp))
    features = mixed.shape[1] * n_tp
    rate = lax.rsqrt(sums[0] / features + epsilon)
    stream_total = sums[3] + 2.0 * rate * sums[2] + rate * rate * sums[1]
    stream_f = (resid_f + gained * rate[:, None]).astype(bf16).astype(f32)
    stream_rate = lax.rsqrt(jnp.maximum(stream_total, 0.0) / features + epsilon)
    normed = (stream_f * stream_rate[:, None] * ffn_gain[None, :]).astype(bf16)

    local_experts = exp_gate.shape[0]
    experts = local_experts * n_sp
    top_count = routes.shape[1]
    capacity = max(1, (3 * rows * top_count + 2 * experts - 1) // (2 * experts))
    flat_routes = routes.reshape(-1)
    onehot = (flat_routes[:, None] == jnp.arange(experts, dtype=jnp.int32)[None, :]).astype(
        jnp.int32
    )
    earlier = jnp.cumsum(onehot, axis=0) - onehot
    slot = flat_routes * capacity + jnp.sum(earlier * onehot, axis=1)
    slots = experts * capacity
    choosers = (
        slot.reshape(rows, top_count)[:, :, None] == jnp.arange(slots, dtype=jnp.int32)
    ).astype(bf16)
    outgoing = jnp.einsum(
        "rs,rc->sc", jnp.sum(choosers, axis=1), normed, preferred_element_type=f32
    ).astype(bf16)
    outgoing = outgoing.reshape(n_sp, local_experts, capacity, normed.shape[1])
    arrived = lax.all_to_all(outgoing, "sp", split_axis=0, concat_axis=0, tiled=True)

    shared_gate = summed(jnp.dot(normed, sh_gate, preferred_element_type=f32).astype(bf16), 1)
    shared_up = summed(jnp.dot(normed, sh_up, preferred_element_type=f32).astype(bf16), 1)
    shared_hidden = joined((jax.nn.silu(shared_gate) * shared_up).astype(bf16), 1)
    shared_out = jnp.dot(shared_hidden, sh_down, preferred_element_type=f32)

    gate_part = jnp.einsum("segd,edf->segf", arrived, exp_gate, preferred_element_type=f32)
    up_part = jnp.einsum("segd,edf->segf", arrived, exp_up, preferred_element_type=f32)
    gate_pre = summed(gate_part.astype(bf16), 3)
    up_pre = summed(up_part.astype(bf16), 3)
    hidden = joined((jax.nn.silu(gate_pre) * up_pre).astype(bf16), 3)
    produced = jnp.einsum("segf,efd->segd", hidden, exp_down, preferred_element_type=f32)
    returned = lax.all_to_all(
        produced.astype(bf16), "sp", split_axis=0, concat_axis=0, tiled=True
    )
    flat_back = returned.reshape(slots, returned.shape[3])
    routed = None
    for k in range(top_count):
        picked = jnp.dot(choosers[:, k], flat_back, preferred_element_type=f32)
        term = gates[:, k : k + 1] * picked
        routed = term if routed is None else routed + term
    return (stream_f + routed + shared_out).astype(bf16)


def solution(mesh):
    return jax.shard_map(
        shards,
        mesh=mesh,
        in_specs=(
            P("sp", "tp"),
            P("sp", "tp"),
            P("sp", "tp"),
            P("sp", "tp"),
            P("sp", "tp"),
            P("sp", "tp"),
            P("sp", "tp"),
            P("sp", "tp"),
            P("tp", None),
            P("tp", None),
            P("sp", "tp"),
            P("tp"),
            P("tp"),
            P("sp", None),
            P("sp", None),
            P("sp", "tp", None),
            P("sp", "tp", None),
            P("sp", None, "tp"),
            P("tp", None),
            P("tp", None),
            P(None, "tp"),
        ),
        out_specs=P("sp", "tp"),
        check_vma=False,
    )
```
